32 devices in a mesh: grp: 2 (over y), sp: 4 (over z), tp: 4 (over x, core).
Axes of the slice: x: 2, y: 2, z: 4, core: 2. Of those that a mesh axis runs over, the one named last changes fastest.
Arguments:
- residual: bfloat16 [1024, 2048], P(('grp', 'sp', 'tp')), parts along dimension 0, may hold values from -6 to 6
- receptance: bfloat16 [1024, 2048], P(('grp', 'sp'), 'tp'), parts along dimension 0, may hold values from -6 to 6
- key_in: bfloat16 [1024, 2048], P(('grp', 'sp'), 'tp'), parts along dimension 0, may hold values from -6 to 6
- value_in: bfloat16 [1024, 2048], P(('grp', 'sp'), 'tp'), parts along dimension 0, may hold values from -6 to 6
- log_decay: float32 [1024, 2048], P(('grp', 'sp'), 'tp'), parts along dimension 0, may hold values from -1 to 0, as said below
- rate_pre: bfloat16 [1024, 2048], P(('grp', 'sp'), 'tp'), parts along dimension 0, may hold values from -11 to 3
- out_gate: bfloat16 [1024, 2048], P(('grp', 'sp'), 'tp'), parts along dimension 0, may hold values from -6 to 6
- group_gain: float32 [2048], P('tp'), may hold values from 0.1 to 1.9
- w_out: bfloat16 [2048, 2048], P('tp'), may hold values from -0.125 to 0.125
- norm_gain: float32 [2048], replicated, may hold values from 0.1 to 1.9
- w_gate: bfloat16 [2048, 5632], P('sp', 'tp'), may hold values from -0.125 to 0.125
- w_value: bfloat16 [2048, 5632], P('sp', 'tp'), may hold values from -0.125 to 0.125
- conv_gate: float32 [3, 5632], P(None, 'tp'), may hold values from -3 to 3
- conv_value: float32 [3, 5632], P(None, 'tp'), may hold values from -3 to 3
- w_down: bfloat16 [5632, 2048], P('tp', 'sp'), may hold values from -0.078125 to 0.078125
Outputs:
- layer_out: bfloat16 [1024, 2048], P(('grp', 'sp', 'tp')), parts along dimension 0
The draws below stay inside these ranges and needn't reach their ends.
There are 2 independent parts, one for each index of `grp`. The reference program is written for one: setup_inputs(seed, part) draws one part's arguments, and reference() takes and returns one part's arrays. A program takes and returns all parts, laid end to end along the dimension named above; an argument that names none is the same for every part. Nothing has to cross between parts.
Inputs may be any that keep to these rules, and one draw needn't show every extreme that they name: `log_decay`: every entry is negative.
All inputs are finite; a program needn't handle non-finite values.
Results may differ from the reference program's by a relative error of at most 0.017.
Values may be sent and summed in bfloat16 or wider, within the bound.
A program may use at most 64 MiB of HBM per device.

```python
import math
import jax
import jax.numpy as jnp
from jax import lax

D = 2048
HEAD = 64
FF = 5632
TOK_DEV = 128
HEADS = 32
TOKENS = 512
N_TP = 4


def draw_log_decay(key, part):
    subkeys = jax.random.split(key, 6)
    fast_share = 0.5
    chosen = jax.random.uniform(subkeys[0], (HEADS,)) < fast_share
    fast_rate = jax.random.uniform(subkeys[1], (HEADS,), minval=1.0 / 100.0, maxval=1.0 / 30.0)
    floor_speed = jnp.where(chosen, fast_rate, 0.3 / TOKENS)
    floor_speed = jnp.repeat(floor_speed, HEAD)
    rough_multiplier = jnp.exp(jax.random.uniform(subkeys[2], (TOKENS, D), minval=-0.7, maxval=0.7))
    multiplier_each_tile = jnp.exp(jax.random.uniform(subkeys[3], (TOKENS // TOK_DEV, HEADS), minval=-0.7, maxval=0.7))
    multiplier_each_tile = jnp.repeat(jnp.repeat(multiplier_each_tile, TOK_DEV, axis=0), HEAD, axis=1)
    third = TOKENS // 3
    place_sequence = jnp.arange(3) * third + jax.random.randint(subkeys[4], (3,), 0, third)
    input_magnitude = jax.random.uniform(subkeys[5], (3,), minval=math.log(0.5), maxval=math.log(0.8))
    element_indices = jnp.arange(TOKENS)
    spike_occurrences = jnp.sum(jnp.where(element_indices[:, None] == place_sequence[None, :], input_magnitude[None, :], 0.0), axis=1)
    return (-floor_speed[None, :] * rough_multiplier * multiplier_each_tile + spike_occurrences[:, None]).astype(jnp.float32)


def draw_rate_pre(key, part):
    subkeys = jax.random.split(key, 3)
    strong_share = 0.25
    noise = jnp.clip(jax.random.normal(subkeys[0], (TOKENS, D)), -3.0, 3.0)
    strong = jax.random.uniform(subkeys[1], (HEADS,)) < strong_share
    weak_level = math.log(HEAD / (3.3 * TOKENS))
    level = jnp.where(strong, 0.0, weak_level)
    block_shift = jax.random.uniform(subkeys[2], (TOKENS // TOK_DEV, HEADS), minval=-0.7, maxval=0.7)
    block_shift = jnp.where(strong[None, :], 0.0, block_shift)
    offsets = level[None, :] + block_shift
    offsets = jnp.repeat(jnp.repeat(offsets, TOK_DEV, axis=0), HEAD, axis=1)
    return (offsets + noise).astype(jnp.float32).astype(jnp.bfloat16)


def steps_of(rng, dims, cuts, least, largest):
    gain, own = 1.0, jax.random.fold_in(rng, 6)
    for axis_at, blocks in cuts:
        steps = jnp.exp(jax.random.uniform(jax.random.fold_in(own, axis_at), (blocks,), jnp.float32, least / len(cuts), largest / len(cuts)))
        gain = gain * jnp.repeat(steps, dims[axis_at] // blocks).reshape([-1 if axis == axis_at else 1 for axis in range(len(dims))])
    return gain


def scatter_about(key, shape, scale, bound, cuts=(), kind=jnp.bfloat16):
    values = jax.random.normal(key, shape, jnp.float32) * scale
    if len(cuts) > 0:
        values = steps_of(key, shape, cuts, -0.22, 0.18) * values
    return jnp.clip(values, min=-bound, max=bound).astype(kind)


def setup_inputs(seed: int = 0, part: int = 0) -> dict:
    keys = jax.random.split(jax.random.key(seed), 16)
    part_splits = jax.random.split(jax.random.fold_in(keys[15], part), 16)
    residual = scatter_about(part_splits[0], (TOKENS, D), 1.0, 6.0, ((0, 16),))
    receptance = scatter_about(part_splits[1], (TOKENS, D), 1.0, 6.0, ((0, 4), (1, 4)))
    key_in = scatter_about(part_splits[2], (TOKENS, D), 1.0, 6.0, ((0, 4), (1, 4)))
    value_in = scatter_about(part_splits[3], (TOKENS, D), 1.0, 6.0, ((0, 4), (1, 4)))
    log_decay = draw_log_decay(jax.random.fold_in(jax.random.fold_in(keys[15], part), 71), part)
    rate_pre = draw_rate_pre(jax.random.fold_in(jax.random.fold_in(keys[15], part), 71), part)
    out_gate = scatter_about(part_splits[6], (TOKENS, D), 1.0, 6.0, ((0, 4), (1, 4)))
    group_gain = jnp.clip(1.0 + 0.18 * jax.random.normal(keys[7], (D,), jnp.float32), 0.1, 1.9)
    w_out = scatter_about(keys[8], (D, D), D ** -0.5, 0.125, ((0, 4),))
    norm_gain = jnp.clip(1.0 + 0.18 * jax.random.normal(keys[9], (D,), jnp.float32), 0.1, 1.9)
    w_gate = scatter_about(keys[10], (D, FF), D ** -0.5, 0.125, ((0, 4), (1, 4)))
    w_value = scatter_about(keys[11], (D, FF), D ** -0.5, 0.125, ((0, 4), (1, 4)))
    conv_gate = scatter_about(keys[12], (3, FF), 0.6, 3.0, ((1, 4),), jnp.float32)
    conv_value = scatter_about(keys[13], (3, FF), 0.6, 3.0, ((1, 4),), jnp.float32)
    w_down = scatter_about(keys[14], (FF, D), FF ** -0.5, 0.078125, ((0, 4), (1, 4)))
    return dict(residual=residual, receptance=receptance, key_in=key_in, value_in=value_in, log_decay=log_decay, rate_pre=rate_pre, out_gate=out_gate, group_gain=group_gain, w_out=w_out, norm_gain=norm_gain, w_gate=w_gate, w_value=w_value, conv_gate=conv_gate, conv_value=conv_value, w_down=w_down)


group_eps = 0.00064
norm_eps = 1e-06
highest = lax.Precision.HIGHEST

def token_step(memory, inputs):
    recept_row, decay_row, key_row, value_row, unit_row, rate_row = inputs
    removed = jnp.einsum('hvk,hk->hv', memory, -unit_row, precision=highest)
    memory = memory * decay_row[:, None, :] + removed[:, :, None] * (unit_row * rate_row)[:, None, :]
    memory = memory + value_row[:, :, None] * key_row[:, None, :]
    output = jnp.einsum('hvk,hk->hv', memory, recept_row, precision=highest)
    return (memory, output)

def group_norm(outputs, group_gain):
    center = lax.optimization_barrier(jnp.mean(outputs, axis=-1, keepdims=True))
    spread = lax.optimization_barrier(jnp.mean(jnp.square(outputs - center), axis=-1, keepdims=True))
    scaled = (outputs - center) * lax.rsqrt(spread + group_eps)
    return scaled * group_gain.astype(jnp.float32).reshape(-1, HEAD)

def blocked_sum(left, right):
    width = left.shape[1] // N_TP
    total = jnp.zeros((left.shape[0], right.shape[1]), jnp.float32)
    for index in range(N_TP):
        part = jnp.dot(left[:, index * width:(index + 1) * width], right[index * width:(index + 1) * width], preferred_element_type=jnp.float32)
        rounded = lax.optimization_barrier(part.astype(jnp.bfloat16))
        total = total + rounded.astype(jnp.float32)
    return total

def causal_conv(upward, taps):
    padded = jnp.pad(upward.astype(jnp.float32), ((2, 0), (0, 0)))
    weights = taps.astype(jnp.float32)
    return weights[0] * padded[:-2] + weights[1] * padded[1:-1] + weights[2] * padded[2:]

def reference(residual, receptance, key_in, value_in, log_decay, rate_pre, out_gate, group_gain, w_out, norm_gain, w_gate, w_value, conv_gate, conv_value, w_down):

    def heads_view(array):
        return array.astype(jnp.float32).reshape(TOKENS, HEADS, HEAD)
    recept = heads_view(receptance)
    keys_all = heads_view(key_in)
    values = heads_view(value_in)
    decays = jnp.exp(heads_view(log_decay))
    rates = jax.nn.sigmoid(heads_view(rate_pre))
    unit_keys = keys_all * lax.rsqrt(lax.optimization_barrier(jnp.sum(keys_all * keys_all, axis=-1, keepdims=True)) + norm_eps)
    start = jnp.zeros((HEADS, HEAD, HEAD), jnp.float32)
    _, mix = lax.scan(token_step, start, (recept, decays, keys_all, values, unit_keys, rates))
    normed_mix = group_norm(mix, group_gain).reshape(TOKENS, D)
    mixed = (normed_mix * out_gate.astype(jnp.float32)).astype(jnp.bfloat16)
    hidden_mid = residual.astype(jnp.float32) + blocked_sum(mixed, w_out)
    scale = lax.rsqrt(lax.optimization_barrier(jnp.mean(hidden_mid * hidden_mid, axis=-1, keepdims=True)) + norm_eps)
    normed_rows = (hidden_mid * scale * norm_gain.astype(jnp.float32)).astype(jnp.bfloat16)
    gate_up = jnp.dot(normed_rows, w_gate, preferred_element_type=jnp.float32).astype(jnp.bfloat16)
    value_up = jnp.dot(normed_rows, w_value, preferred_element_type=jnp.float32).astype(jnp.bfloat16)
    gate_conv = causal_conv(gate_up, conv_gate)
    value_conv = causal_conv(value_up, conv_value)
    hidden_ffn = (jax.nn.silu(gate_conv) * value_conv).astype(jnp.bfloat16)
    return (hidden_mid + blocked_sum(hidden_ffn, w_down)).astype(jnp.bfloat16)
```

```python
import functools

import jax
import jax.numpy as jnp
from jax import lax
from jax.experimental import pallas as pl
from jax.experimental.pallas import tpu as pltpu
from jax.sharding import PartitionSpec as P

HEAD = 64
HALO = 16
group_eps = 0.00064
norm_eps = 1e-06
f32 = jnp.float32
bf16 = jnp.bfloat16
MESH = pl.DeviceIdType.MESH


def dot(a, b, dims=((1,), (0,))):
    return lax.dot_general(
        a, b, (dims, ((), ())), precision=lax.Precision.HIGHEST, preferred_element_type=f32
    )


def fast_dot(a, b):
    return jnp.dot(a, b, preferred_element_type=f32)


def inverse(tri, row, col):
    count = tri.shape[0]
    eye = (row == col).astype(f32)
    small = jnp.where(row // 8 == col // 8, tri, 0.0)
    second = dot(small, small)
    fourth = dot(second, second)
    inv = eye - small
    inv = inv + dot(inv, second)
    inv = inv + dot(inv, fourth)
    size = 16
    while size <= count:
        off = jnp.where(
            (row // size == col // size) & (row // (size // 2) != col // (size // 2)), tri, 0.0
        )
        inv = inv - dot(inv, dot(off, inv))
        size *= 2
    return inv


def body(
    S,
    T,
    recept_ref,
    key_ref,
    value_ref,
    decay_ref,
    rate_ref,
    gate_ref,
    gain_ref,
    resid_ref,
    norm_ref,
    taps_g_ref,
    taps_v_ref,
    wo_hbm,
    wg_hbm,
    wv_hbm,
    wd_hbm,
    out_ref,
    wo,
    wg,
    wv,
    wd,
    q_buf,
    o_buf,
    g_buf,
    u_buf,
    enter_buf,
    leave_buf,
    mixed_buf,
    attn_part,
    attn_recv,
    mid_buf,
    norm_send,
    x_buf,
    up_part,
    up_recv,
    up_acc,
    hid_buf,
    down_part,
    down_recv,
    w_sem,
    chain_sem,
    attn_s,
    attn_r,
    x_s,
    x_r,
    up_s,
    up_r,
    hid_s,
    hid_r,
    down_s,
    down_r,
):
    s, t = lax.axis_index("sp"), lax.axis_index("tp")
    me = s * T + t
    N = S * T
    tok, width = recept_ref.shape
    heads = width // HEAD
    R = resid_ref.shape[0]
    K = x_buf.shape[1]

    loads = [
        pltpu.make_async_copy(a, b, w_sem.at[i])
        for i, (a, b) in enumerate(((wo_hbm, wo), (wg_hbm, wg), (wv_hbm, wv), (wd_hbm, wd)))
    ]
    for load in loads:
        load.start()

    barrier = pltpu.get_barrier_semaphore()

    def greet(d, c):
        peer = lax.rem(me + d, N)
        pl.semaphore_signal(
            barrier,
            inc=1,
            device_id={"sp": peer // T, "tp": lax.rem(peer, T)},
            device_id_type=MESH,
        )
        return c

    lax.fori_loop(1, N, greet, 0)

    row = lax.broadcasted_iota(jnp.int32, (tok, tok), 0)
    col = lax.broadcasted_iota(jnp.int32, (tok, tok), 1)
    lower = (row >= col).astype(f32)
    logs = decay_ref[...]
    total = dot(lower, logs)
    middle = total[tok // 2 - 1 : tok // 2, :]
    last = total[tok - 1 : tok, :]
    earlier = total - logs
    hrow = lax.broadcasted_iota(jnp.int32, (HEAD, HEAD), 0)
    hcol = lax.broadcasted_iota(jnp.int32, (HEAD, HEAD), 1)
    for h in range(heads):
        cols = slice(h * HEAD, (h + 1) * HEAD)
        keys = key_ref[:, cols].astype(f32)
        unit = keys * lax.rsqrt(jnp.sum(keys * keys, axis=-1, keepdims=True) + norm_eps)
        push = unit * jax.nn.sigmoid(rate_ref[:, cols].astype(f32))
        vals = value_ref[:, cols].astype(f32)
        rec = recept_ref[:, cols].astype(f32)
        tot, mid, lst, ear = total[:, cols], middle[:, cols], last[:, cols], earlier[:, cols]
        up = jnp.exp(mid - tot)
        to_end = jnp.exp(lst - tot)
        lefts = jnp.concatenate([unit * jnp.exp(ear - mid), rec * jnp.exp(tot - mid)], axis=0)
        rights = jnp.concatenate([push * up, keys * up], axis=0)
        inner = dot(lefts, rights, ((1,), (1,)))
        a_pb = jnp.where(row > col, inner[:tok, :tok], 0.0)
        a_pk = jnp.where(row > col, inner[:tok, tok:], 0.0)
        a_rb = jnp.where(row >= col, inner[tok:, :tok], 0.0)
        a_rk = jnp.where(row >= col, inner[tok:, tok:], 0.0)
        pk_v = dot(a_pk, vals)
        inv = inverse(a_pb, row, col)
        solved = dot(inv, jnp.concatenate([unit * jnp.exp(ear), pk_v], axis=1))
        read = dot(a_rb, solved)
        q_buf[:, cols] = rec * jnp.exp(tot) - read[:, :HEAD]
        o_buf[:, cols] = dot(a_rk, vals) - read[:, HEAD:]
        back = dot(solved, push * to_end, ((0,), (0,)))
        g_buf[h] = jnp.where(hrow == hcol, jnp.exp(lst), 0.0) - back[:HEAD]
        u_buf[h] = dot(vals, keys * to_end, ((0,), (0,))) - back[HEAD:]

    pl.semaphore_wait(barrier, N - 1)

    chain = pltpu.make_async_remote_copy(
        src_ref=leave_buf,
        dst_ref=enter_buf,
        send_sem=chain_sem.at[0],
        recv_sem=chain_sem.at[1],
        device_id={"sp": jnp.minimum(s + 1, S - 1), "tp": t},
        device_id_type=MESH,
    )

    @pl.when(s == 0)
    def _():
        enter_buf[...] = jnp.zeros_like(enter_buf)

    @pl.when(s > 0)
    def _():
        chain.wait_recv()

    @pl.when(s < S - 1)
    def _():
        for h in range(heads):
            rows = slice((h // 2) * HEAD, (h // 2 + 1) * HEAD)
            lanes = slice((h % 2) * HEAD, (h % 2 + 1) * HEAD)
            state = dot(enter_buf[rows, lanes].astype(f32), g_buf[h]) + u_buf[h]
            leave_buf[rows, lanes] = state.astype(bf16)
        chain.start()

    for h in range(heads):
        cols = slice(h * HEAD, (h + 1) * HEAD)
        rows = slice((h // 2) * HEAD, (h // 2 + 1) * HEAD)
        lanes = slice((h % 2) * HEAD, (h % 2 + 1) * HEAD)
        mix = o_buf[:, cols] + dot(
            q_buf[:, cols], enter_buf[rows, lanes].astype(f32), ((1,), (1,))
        )
        away = mix - jnp.mean(mix, axis=-1, keepdims=True)
        spread = jnp.mean(away * away, axis=-1, keepdims=True)
        normed = away * lax.rsqrt(spread + group_eps) * gain_ref[:, cols]
        mixed_buf[:, cols] = (normed * gate_ref[:, cols].astype(f32)).astype(bf16)

    loads[0].wait()
    attn_part[...] = fast_dot(mixed_buf[...], wo[...]).astype(bf16)
    own_rows = pl.ds(pl.multiple_of(t * R, R), R)
    sends = []
    for d in range(1, T):
        to = lax.rem(t + d, T)
        sends.append(
            pltpu.make_async_remote_copy(
                src_ref=attn_part.at[pl.ds(pl.multiple_of(to * R, R), R)],
                dst_ref=attn_recv.at[d],
                send_sem=attn_s.at[d],
                recv_sem=attn_r.at[d],
                device_id={"sp": s, "tp": to},
                device_id_type=MESH,
            )
        )
        sends[-1].start()
    hidden = resid_ref[...].astype(f32) + attn_part[own_rows, :].astype(f32)
    for d in range(1, T):
        sends[d - 1].wait_recv()
        hidden = hidden + attn_recv[d].astype(f32)
    mid_buf[...] = hidden
    scale = lax.rsqrt(jnp.mean(hidden * hidden, axis=-1, keepdims=True) + norm_eps)
    normed = (hidden * scale * norm_ref[...]).astype(bf16)
    for i in range(S):
        norm_send[i] = normed[:, i * K : (i + 1) * K]

    x_buf[:HALO, :] = jnp.zeros((HALO, K), bf16)
    my_x = pl.ds(pl.multiple_of(HALO + me * R, 16), R)

    def x_copy(peer, slot):
        return pltpu.make_async_remote_copy(
            src_ref=norm_send.at[peer // T],
            dst_ref=x_buf.at[my_x],
            send_sem=x_s.at[slot],
            recv_sem=x_r.at[slot],
            device_id={"sp": peer // T, "tp": lax.rem(peer, T)},
            device_id_type=MESH,
        )

    def x_send(d, c):
        x_copy(lax.rem(me + d, N), d).start()
        return c

    lax.fori_loop(1, N, x_send, 0)
    x_buf[my_x, :] = norm_send[s]

    def x_wait(d, c):
        copy = x_copy(lax.rem(me + d, N), d)
        copy.wait_recv()
        copy.wait_send()
        return c

    lax.fori_loop(1, N, x_wait, 0)

    loads[1].wait()
    loads[2].wait()

    def up_copy(d):
        to = lax.rem(s + d, S)
        return pltpu.make_async_remote_copy(
            src_ref=up_part.at[d],
            dst_ref=up_recv.at[d],
            send_sem=up_s.at[d],
            recv_sem=up_r.at[d],
            device_id={"sp": to, "tp": t},
            device_id_type=MESH,
        )

    def up_rows(to):
        return x_buf[pl.ds(pl.multiple_of(to * tok, 16), tok + HALO), :]

    def up_send(d, c):
        rows = up_rows(lax.rem(s + d, S))
        up_part[d, 0] = fast_dot(rows, wg[...]).astype(bf16)
        up_part[d, 1] = fast_dot(rows, wv[...]).astype(bf16)
        up_copy(d).start()
        return c

    lax.fori_loop(1, S, up_send, 0)
    rows = up_rows(s)
    up_acc[0] = fast_dot(rows, wg[...])
    up_acc[1] = fast_dot(rows, wv[...])

    def up_take(d, c):
        copy = up_copy(d)
        copy.wait_recv()
        up_acc[...] = up_acc[...] + up_recv[d].astype(f32)
        return c

    lax.fori_loop(1, S, up_take, 0)

    def conv(which, taps):
        full = up_acc[which].astype(bf16).astype(f32)
        return (
            taps[0:1, :] * full[HALO - 2 : HALO - 2 + tok]
            + taps[1:2, :] * full[HALO - 1 : HALO - 1 + tok]
            + taps[2:3, :] * full[HALO : HALO + tok]
        )

    gated = conv(0, taps_g_ref)
    my_hid = pl.ds(pl.multiple_of(s * tok, tok), tok)
    hid_buf[my_hid, :] = (gated / (1.0 + jnp.exp(-gated)) * conv(1, taps_v_ref)).astype(bf16)

    def hid_copy(d):
        to = lax.rem(s + d, S)
        return pltpu.make_async_remote_copy(
            src_ref=hid_buf.at[my_hid],
            dst_ref=hid_buf.at[my_hid],
            send_sem=hid_s.at[d],
            recv_sem=hid_r.at[d],
            device_id={"sp": to, "tp": t},
            device_id_type=MESH,
        )

    def hid_send(d, c):
        hid_copy(d).start()
        return c

    lax.fori_loop(1, S, hid_send, 0)
    loads[3].wait()

    def down_copy(peer, slot):
        return pltpu.make_async_remote_copy(
            src_ref=down_part.at[pl.ds(pl.multiple_of(peer * R, R), R)],
            dst_ref=down_recv.at[me],
            send_sem=down_s.at[slot],
            recv_sem=down_r.at[slot],
            device_id={"sp": peer // T, "tp": lax.rem(peer, T)},
            device_id_type=MESH,
        )

    def down_block(frm):
        block = pl.ds(pl.multiple_of(frm * tok, tok), tok)
        down_part[block, :] = fast_dot(hid_buf[block, :], wd[...]).astype(bf16)

    down_block(s)
    for j in range(1, T):
        down_copy(s * T + lax.rem(t + j, T), j).start()

    def down_step(d, c):
        hid_copy(d).wait_recv()
        frm = lax.rem(s + S - d, S)
        down_block(frm)

        def one(j, c2):
            down_copy(frm * T + lax.rem(t + j, T), d * T + j).start()
            return c2

        lax.fori_loop(0, T, one, 0)
        return c

    lax.fori_loop(1, S, down_step, 0)
    down_recv[me] = down_part[pl.ds(pl.multiple_of(me * R, R), R), :]

    def down_wait(e, c):
        frm = lax.rem(s + S - e // T, S)
        copy = down_copy(frm * T + lax.rem(t + lax.rem(e, T), T), e)
        copy.wait_recv()
        copy.wait_send()
        return c

    lax.fori_loop(1, N, down_wait, 0)
    for i in range(S):
        lanes = slice(i * K, (i + 1) * K)
        summed = down_recv[i * T].astype(f32)
        for j in range(1, T):
            summed = summed + down_recv[i * T + j].astype(f32)
        out_ref[:, lanes] = (mid_buf[:, lanes] + summed).astype(bf16)

    for send in sends:
        send.wait_send()

    def finish(d, c):
        up_copy(d).wait_send()
        hid_copy(d).wait_send()
        return c

    lax.fori_loop(1, S, finish, 0)

    @pl.when(s < S - 1)
    def _():
        chain.wait_send()


def shards(S, T, *args):
    (
        residual,
        receptance,
        key_in,
        value_in,
        log_decay,
        rate_pre,
        out_gate,
        group_gain,
        w_out,
        norm_gain,
        w_gate,
        w_value,
        conv_gate,
        conv_value,
        w_down,
    ) = args
    tok, width = receptance.shape
    heads = width // HEAD
    R, D = residual.shape
    K, F = w_gate.shape
    N = S * T
    vmem = pl.BlockSpec(memory_space=pltpu.VMEM)
    hbm = pl.BlockSpec(memory_space=pl.ANY)
    dma = pltpu.SemaphoreType.DMA
    packed = ((heads + 1) // 2 * HEAD, 2 * HEAD)
    return pl.pallas_call(
        functools.partial(body, S, T),
        out_shape=jax.ShapeDtypeStruct((R, D), bf16),
        in_specs=[vmem] * 11 + [hbm] * 4,
        out_specs=vmem,
        scratch_shapes=[
            pltpu.VMEM(w_out.shape, bf16),
            pltpu.VMEM(w_gate.shape, bf16),
            pltpu.VMEM(w_value.shape, bf16),
            pltpu.VMEM(w_down.shape, bf16),
            pltpu.VMEM((tok, width), f32),
            pltpu.VMEM((tok, width), f32),
            pltpu.VMEM((heads, HEAD, HEAD), f32),
            pltpu.VMEM((heads, HEAD, HEAD), f32),
            pltpu.VMEM(packed, bf16),
            pltpu.VMEM(packed, bf16),
            pltpu.VMEM((tok, width), bf16),
            pltpu.VMEM((tok, D), bf16),
            pltpu.VMEM((T, R, D), bf16),
            pltpu.VMEM((R, D), f32),
            pltpu.VMEM((S, R, K), bf16),
            pltpu.VMEM((HALO + N * R, K), bf16),
            pltpu.VMEM((S, 2, tok + HALO, F), bf16),
            pltpu.VMEM((S, 2, tok + HALO, F), bf16),
            pltpu.VMEM((2, tok + HALO, F), f32),
            pltpu.VMEM((S * tok, F), bf16),
            pltpu.VMEM((N * R, K), bf16),
            pltpu.VMEM((N, R, K), bf16),
            dma((4,)),
            dma((2,)),
            dma((T,)),
            dma((T,)),
            dma((N,)),
            dma((N,)),
            dma((S,)),
            dma((S,)),
            dma((S,)),
            dma((S,)),
            dma((N,)),
            dma((N,)),
        ],
        compiler_params=pltpu.CompilerParams(collective_id=0, has_side_effects=True),
    )(
        receptance,
        key_in,
        value_in,
        log_decay,
        rate_pre,
        out_gate,
        group_gain.reshape(1, -1),
        residual,
        norm_gain.reshape(1, -1),
        conv_gate,
        conv_value,
        w_out,
        w_gate,
        w_value,
        w_down,
    )


def solution(mesh):
    in_specs = (
        P(("grp", "sp", "tp"), None),
        P(("grp", "sp"), "tp"),
        P(("grp", "sp"), "tp"),
        P(("grp", "sp"), "tp"),
        P(("grp", "sp"), "tp"),
        P(("grp", "sp"), "tp"),
        P(("grp", "sp"), "tp"),
        P("tp"),
        P("tp", None),
        P(),
        P("sp", "tp"),
        P("sp", "tp"),
        P(None, "tp"),
        P(None, "tp"),
        P("tp", "sp"),
    )
    out_specs = P(("grp", "sp", "tp"), None)
    return jax.shard_map(
        functools.partial(shards, mesh.shape["sp"], mesh.shape["tp"]),
        mesh=mesh,
        in_specs=in_specs,
        out_specs=out_specs,
        check_vma=False,
    )
```

```python
import functools

import jax
import jax.numpy as jnp
from jax import lax
from jax.experimental import pallas as pl
from jax.experimental.pallas import tpu as pltpu
from jax.sharding import PartitionSpec as P

HEAD = 64
HALO = 16
group_eps = 0.00064
norm_eps = 1e-06
f32 = jnp.float32
bf16 = jnp.bfloat16
MESH = pl.DeviceIdType.MESH


def dot(a, b, dims=((1,), (0,))):
    return lax.dot_general(
        a, b, (dims, ((), ())), precision=lax.Precision.HIGHEST, preferred_element_type=f32
    )


def fast_dot(a, b):
    return jnp.dot(a, b, preferred_element_type=f32)


def inverse(tri, row, col):
    count = tri.shape[0]
    eye = (row == col).astype(f32)
    small = jnp.where(row // 8 == col // 8, tri, 0.0)
    second = dot(small, small)
    fourth = dot(second, second)
    inv = eye - small
    inv = inv + dot(inv, second)
    inv = inv + dot(inv, fourth)
    size = 16
    while size <= count:
        off = jnp.where(
            (row // size == col // size) & (row // (size // 2) != col // (size // 2)), tri, 0.0
        )
        inv = inv - dot(inv, dot(off, inv))
        size *= 2
    return inv


def body(
    S,
    T,
    recept_ref,
    key_ref,
    value_ref,
    decay_ref,
    rate_ref,
    gate_ref,
    gain_ref,
    resid_ref,
    norm_ref,
    taps_g_ref,
    taps_v_ref,
    wo_hbm,
    wg_hbm,
    wv_hbm,
    wd_hbm,
    out_ref,
    wo,
    wup,
    wd,
    q_buf,
    o_buf,
    g_buf,
    u_buf,
    enter_buf,
    leave_buf,
    mixed_buf,
    attn_part,
    attn_recv,
    mid_buf,
    norm_send,
    x_buf,
    up_part,
    up_recv,
    up_acc,
    hid_buf,
    down_part,
    down_recv,
    w_sem,
    chain_sem,
    attn_s,
    attn_r,
    xz_s,
    xz_r,
    xt_s,
    xt_r,
    up_s,
    up_r,
    hid_s,
    hid_r,
    down_s,
    down_r,
):
    s, t = lax.axis_index("sp"), lax.axis_index("tp")
    me = s * T + t
    N = S * T
    tok, width = recept_ref.shape
    heads = width // HEAD
    R = resid_ref.shape[0]
    K = wd.shape[1]
    par = lax.rem(s, 2)

    my_k = pl.ds(pl.multiple_of(par * K, K), K)
    loads = [
        pltpu.make_async_copy(a, b, w_sem.at[i]) for i, (a, b) in enumerate(((wo_hbm, wo), (wd_hbm, wd)))
    ]
    for load in loads:
        load.start()

    def swap(own, other):
        keep = pltpu.make_async_copy(own, wup.at[my_k], w_sem.at[2])
        give = pltpu.make_async_remote_copy(
            src_ref=other,
            dst_ref=wup.at[my_k],
            send_sem=w_sem.at[3],
            recv_sem=w_sem.at[4],
            device_id={"sp": s + 1 - 2 * par, "tp": t},
            device_id_type=MESH,
        )
        return keep, give

    barrier = pltpu.get_barrier_semaphore()

    def greet(d, c):
        peer = lax.rem(me + d, N)
        pl.semaphore_signal(
            barrier,
            inc=1,
            device_id={"sp": peer // T, "tp": lax.rem(peer, T)},
            device_id_type=MESH,
        )
        return c

    lax.fori_loop(1, N, greet, 0)
    pl.semaphore_wait(barrier, N - 1)

    @pl.when(par == 0)
    def _():
        for copy in swap(wg_hbm, wv_hbm):
            copy.start()

    @pl.when(par == 1)
    def _():
        for copy in swap(wv_hbm, wg_hbm):
            copy.start()

    row = lax.broadcasted_iota(jnp.int32, (tok, tok), 0)
    col = lax.broadcasted_iota(jnp.int32, (tok, tok), 1)
    lower = (row >= col).astype(f32)
    logs = decay_ref[...]
    total = dot(lower, logs)
    middle = total[tok // 2 - 1 : tok // 2, :]
    last = total[tok - 1 : tok, :]
    earlier = total - logs
    hrow = lax.broadcasted_iota(jnp.int32, (HEAD, HEAD), 0)
    hcol = lax.broadcasted_iota(jnp.int32, (HEAD, HEAD), 1)
    for h in range(heads):
        cols = slice(h * HEAD, (h + 1) * HEAD)
        keys = key_ref[:, cols].astype(f32)
        unit = keys * lax.rsqrt(jnp.sum(keys * keys, axis=-1, keepdims=True) + norm_eps)
        push = unit * jax.nn.sigmoid(rate_ref[:, cols].astype(f32))
        vals = value_ref[:, cols].astype(f32)
        rec = recept_ref[:, cols].astype(f32)
        tot, mid, lst, ear = total[:, cols], middle[:, cols], last[:, cols], earlier[:, cols]
        up = jnp.exp(mid - tot)
        to_end = jnp.exp(lst - tot)
        lefts = jnp.concatenate([unit * jnp.exp(ear - mid), rec * jnp.exp(tot - mid)], axis=0)
        rights = jnp.concatenate([push * up, keys * up], axis=0)
        inner = dot(lefts, rights, ((1,), (1,)))
        a_pb = jnp.where(row > col, inner[:tok, :tok], 0.0)
        a_pk = jnp.where(row > col, inner[:tok, tok:], 0.0)
        a_rb = jnp.where(row >= col, inner[tok:, :tok], 0.0)
        a_rk = jnp.where(row >= col, inner[tok:, tok:], 0.0)
        pk_v = dot(a_pk, vals)
        inv = inverse(a_pb, row, col)
        solved = dot(inv, jnp.concatenate([unit * jnp.exp(ear), pk_v], axis=1))
        read = dot(a_rb, solved)
        q_buf[:, cols] = rec * jnp.exp(tot) - read[:, :HEAD]
        o_buf[:, cols] = dot(a_rk, vals) - read[:, HEAD:]
        back = dot(solved, push * to_end, ((0,), (0,)))
        g_buf[h] = jnp.where(hrow == hcol, jnp.exp(lst), 0.0) - back[:HEAD]
        u_buf[h] = dot(vals, keys * to_end, ((0,), (0,))) - back[HEAD:]

    chain = pltpu.make_async_remote_copy(
        src_ref=leave_buf,
        dst_ref=enter_buf,
        send_sem=chain_sem.at[0],
        recv_sem=chain_sem.at[1],
        device_id={"sp": jnp.minimum(s + 1, S - 1), "tp": t},
        device_id_type=MESH,
    )

    @pl.when(s == 0)
    def _():
        enter_buf[...] = jnp.zeros_like(enter_buf)

    @pl.when(s > 0)
    def _():
        chain.wait_recv()

    @pl.when(s < S - 1)
    def _():
        for h in range(heads):
            rows = slice((h // 2) * HEAD, (h // 2 + 1) * HEAD)
            lanes = slice((h % 2) * HEAD, (h % 2 + 1) * HEAD)
            state = dot(enter_buf[rows, lanes].astype(f32), g_buf[h]) + u_buf[h]
            leave_buf[rows, lanes] = state.astype(bf16)
        chain.start()

    for h in range(heads):
        cols = slice(h * HEAD, (h + 1) * HEAD)
        rows = slice((h // 2) * HEAD, (h // 2 + 1) * HEAD)
        lanes = slice((h % 2) * HEAD, (h % 2 + 1) * HEAD)
        mix = o_buf[:, cols] + dot(
            q_buf[:, cols], enter_buf[rows, lanes].astype(f32), ((1,), (1,))
        )
        away = mix - jnp.mean(mix, axis=-1, keepdims=True)
        spread = jnp.mean(away * away, axis=-1, keepdims=True)
        normed = away * lax.rsqrt(spread + group_eps) * gain_ref[:, cols]
        mixed_buf[:, cols] = (normed * gate_ref[:, cols].astype(f32)).astype(bf16)

    loads[0].wait()
    attn_part[...] = fast_dot(mixed_buf[...], wo[...]).astype(bf16)
    own_rows = pl.ds(pl.multiple_of(t * R, R), R)
    sends = []
    for d in range(1, T):
        to = lax.rem(t + d, T)
        sends.append(
            pltpu.make_async_remote_copy(
                src_ref=attn_part.at[pl.ds(pl.multiple_of(to * R, R), R)],
                dst_ref=attn_recv.at[d],
                send_sem=attn_s.at[d],
                recv_sem=attn_r.at[d],
                device_id={"sp": s, "tp": to},
                device_id_type=MESH,
            )
        )
        sends[-1].start()
    hidden = resid_ref[...].astype(f32) + attn_part[own_rows, :].astype(f32)
    for d in range(1, T):
        sends[d - 1].wait_recv()
        hidden = hidden + attn_recv[d].astype(f32)
    mid_buf[...] = hidden
    scale = lax.rsqrt(jnp.mean(hidden * hidden, axis=-1, keepdims=True) + norm_eps)
    normed = (hidden * scale * norm_ref[...]).astype(bf16)
    for i in range(S // 2):
        norm_send[i] = normed[:, i * 2 * K : (i + 1) * 2 * K]

    x_buf[:HALO, :] = jnp.zeros((HALO, 2 * K), bf16)

    def x_rows(place, part):
        return pl.ds(pl.multiple_of(HALO + (place * T + part) * R, 16), R)

    def xz_copy(d):
        to = lax.rem(s + d, S)
        return pltpu.make_async_remote_copy(
            src_ref=norm_send.at[to // 2],
            dst_ref=x_buf.at[x_rows(s, t)],
            send_sem=xz_s.at[d],
            recv_sem=xz_r.at[d],
            device_id={"sp": to, "tp": t},
            device_id_type=MESH,
        )

    def xt_copy(d, j, src, rows):
        return pltpu.make_async_remote_copy(
            src_ref=src,
            dst_ref=x_buf.at[rows],
            send_sem=xt_s.at[d * T + j],
            recv_sem=xt_r.at[d * T + j],
            device_id={"sp": s, "tp": lax.rem(t + j, T)},
            device_id_type=MESH,
        )

    def xz_send(d, c):
        xz_copy(d).start()
        return c

    lax.fori_loop(1, S, xz_send, 0)
    for j in range(1, T):
        xt_copy(0, j, norm_send.at[s // 2], x_rows(s, t)).start()
    x_buf[x_rows(s, t), :] = norm_send[s // 2]

    def x_pass(d, c):
        xz_copy(d).wait_recv()
        rows = x_rows(lax.rem(s + S - d, S), t)
        for j in range(1, T):
            xt_copy(d, j, x_buf.at[rows], rows).start()
        return c

    lax.fori_loop(1, S, x_pass, 0)

    def xt_wait(d, c):
        rows = x_rows(lax.rem(s + S - d, S), t)
        for j in range(1, T):
            copy = xt_copy(d, j, x_buf.at[rows], rows)
            copy.wait_recv()
            copy.wait_send()
        return c

    lax.fori_loop(0, S, xt_wait, 0)

    @pl.when(par == 0)
    def _():
        for copy in swap(wg_hbm, wv_hbm):
            copy.wait()

    @pl.when(par == 1)
    def _():
        for copy in swap(wv_hbm, wg_hbm):
            copy.wait()

    def up_copy(d):
        to = lax.rem(s + d, S)
        return pltpu.make_async_remote_copy(
            src_ref=up_part.at[d],
            dst_ref=up_recv.at[d],
            send_sem=up_s.at[d],
            recv_sem=up_r.at[d],
            device_id={"sp": to, "tp": t},
            device_id_type=MESH,
        )

    def up_rows(to):
        return x_buf[pl.ds(pl.multiple_of(to * tok, 16), tok + HALO), :]

    def up_send(d, c):
        up_part[d] = fast_dot(up_rows(lax.rem(s + d, S)), wup[...]).astype(bf16)
        up_copy(d).start()
        return c

    lax.fori_loop(1, S, up_send, 0)
    up_acc[par] = fast_dot(up_rows(s), wup[...])
    up_acc[1 - par] = jnp.zeros(up_acc.shape[1:], f32)

    def up_take(d, c):
        up_copy(d).wait_recv()
        which = lax.rem(s + S - d, 2)
        up_acc[which] = up_acc[which] + up_recv[d].astype(f32)
        return c

    lax.fori_loop(1, S, up_take, 0)

    def conv(which, taps):
        full = up_acc[which].astype(bf16).astype(f32)
        return (
            taps[0:1, :] * full[HALO - 2 : HALO - 2 + tok]
            + taps[1:2, :] * full[HALO - 1 : HALO - 1 + tok]
            + taps[2:3, :] * full[HALO : HALO + tok]
        )

    gated = conv(0, taps_g_ref)
    my_hid = pl.ds(pl.multiple_of(s * tok, tok), tok)
    hid_buf[my_hid, :] = (gated / (1.0 + jnp.exp(-gated)) * conv(1, taps_v_ref)).astype(bf16)

    def hid_copy(d):
        to = lax.rem(s + d, S)
        return pltpu.make_async_remote_copy(
            src_ref=hid_buf.at[my_hid],
            dst_ref=hid_buf.at[my_hid],
            send_sem=hid_s.at[d],
            recv_sem=hid_r.at[d],
            device_id={"sp": to, "tp": t},
            device_id_type=MESH,
        )

    def hid_send(d, c):
        hid_copy(d).start()
        return c

    lax.fori_loop(1, S, hid_send, 0)
    loads[1].wait()

    def down_copy(peer, slot):
        return pltpu.make_async_remote_copy(
            src_ref=down_part.at[pl.ds(pl.multiple_of(peer * R, R), R)],
            dst_ref=down_recv.at[me],
            send_sem=down_s.at[slot],
            recv_sem=down_r.at[slot],
            device_id={"sp": peer // T, "tp": lax.rem(peer, T)},
            device_id_type=MESH,
        )

    def down_block(frm):
        block = pl.ds(pl.multiple_of(frm * tok, tok), tok)
        down_part[block, :] = fast_dot(hid_buf[block, :], wd[...]).astype(bf16)

    down_block(s)
    for j in range(1, T):
        down_copy(s * T + lax.rem(t + j, T), j).start()

    def down_step(d, c):
        hid_copy(d).wait_recv()
        frm = lax.rem(s + S - d, S)
        down_block(frm)

        def one(j, c2):
            down_copy(frm * T + lax.rem(t + j, T), d * T + j).start()
            return c2

        lax.fori_loop(0, T, one, 0)
        return c

    lax.fori_loop(1, S, down_step, 0)
    down_recv[me] = down_part[pl.ds(pl.multiple_of(me * R, R), R), :]

    def down_wait(e, c):
        frm = lax.rem(s + S - e // T, S)
        copy = down_copy(frm * T + lax.rem(t + lax.rem(e, T), T), e)
        copy.wait_recv()
        copy.wait_send()
        return c

    lax.fori_loop(1, N, down_wait, 0)
    for i in range(S):
        lanes = slice(i * K, (i + 1) * K)
        summed = down_recv[i * T].astype(f32)
        for j in range(1, T):
            summed = summed + down_recv[i * T + j].astype(f32)
        out_ref[:, lanes] = (mid_buf[:, lanes] + summed).astype(bf16)

    for send in sends:
        send.wait_send()

    def finish(d, c):
        xz_copy(d).wait_send()
        up_copy(d).wait_send()
        hid_copy(d).wait_send()
        return c

    lax.fori_loop(1, S, finish, 0)

    @pl.when(s < S - 1)
    def _():
        chain.wait_send()


def shards(S, T, *args):
    (
        residual,
        receptance,
        key_in,
        value_in,
        log_decay,
        rate_pre,
        out_gate,
        group_gain,
        w_out,
        norm_gain,
        w_gate,
        w_value,
        conv_gate,
        conv_value,
        w_down,
    ) = args
    tok, width = receptance.shape
    heads = width // HEAD
    R, D = residual.shape
    K, F = w_gate.shape
    N = S * T
    vmem = pl.BlockSpec(memory_space=pltpu.VMEM)
    hbm = pl.BlockSpec(memory_space=pl.ANY)
    dma = pltpu.SemaphoreType.DMA
    packed = ((heads + 1) // 2 * HEAD, 2 * HEAD)
    return pl.pallas_call(
        functools.partial(body, S, T),
        out_shape=jax.ShapeDtypeStruct((R, D), bf16),
        in_specs=[vmem] * 11 + [hbm] * 4,
        out_specs=vmem,
        scratch_shapes=[
            pltpu.VMEM(w_out.shape, bf16),
            pltpu.VMEM((2 * K, F), bf16),
            pltpu.VMEM(w_down.shape, bf16),
            pltpu.VMEM((tok, width), f32),
            pltpu.VMEM((tok, width), f32),
            pltpu.VMEM((heads, HEAD, HEAD), f32),
            pltpu.VMEM((heads, HEAD, HEAD), f32),
            pltpu.VMEM(packed, bf16),
            pltpu.VMEM(packed, bf16),
            pltpu.VMEM((tok, width), bf16),
            pltpu.VMEM((tok, D), bf16),
            pltpu.VMEM((T, R, D), bf16),
            pltpu.VMEM((R, D), f32),
            pltpu.VMEM((S // 2, R, 2 * K), bf16),
            pltpu.VMEM((HALO + N * R, 2 * K), bf16),
            pltpu.VMEM((S, tok + HALO, F), bf16),
            pltpu.VMEM((S, tok + HALO, F), bf16),
            pltpu.VMEM((2, tok + HALO, F), f32),
            pltpu.VMEM((S * tok, F), bf16),
            pltpu.VMEM((N * R, K), bf16),
            pltpu.VMEM((N, R, K), bf16),
            dma((5,)),
            dma((2,)),
            dma((T,)),
            dma((T,)),
            dma((S,)),
            dma((S,)),
            dma((N,)),
            dma((N,)),
            dma((S,)),
            dma((S,)),
            dma((S,)),
            dma((S,)),
            dma((N,)),
            dma((N,)),
        ],
        compiler_params=pltpu.CompilerParams(collective_id=0, has_side_effects=True),
    )(
        receptance,
        key_in,
        value_in,
        log_decay,
        rate_pre,
        out_gate,
        group_gain.reshape(1, -1),
        residual,
        norm_gain.reshape(1, -1),
        conv_gate,
        conv_value,
        w_out,
        w_gate,
        w_value,
        w_down,
    )


def solution(mesh):
    in_specs = (
        P(("grp", "sp", "tp"), None),
        P(("grp", "sp"), "tp"),
        P(("grp", "sp"), "tp"),
        P(("grp", "sp"), "tp"),
        P(("grp", "sp"), "tp"),
        P(("grp", "sp"), "tp"),
        P(("grp", "sp"), "tp"),
        P("tp"),
        P("tp", None),
        P(),
        P("sp", "tp"),
        P("sp", "tp"),
        P(None, "tp"),
        P(None, "tp"),
        P("tp", "sp"),
    )
    out_specs = P(("grp", "sp", "tp"), None)
    return jax.shard_map(
        functools.partial(shards, mesh.shape["sp"], mesh.shape["tp"]),
        mesh=mesh,
        in_specs=in_specs,
        out_specs=out_specs,
        check_vma=False,
    )
```
